128 devices in a mesh: sp: 32 (over z, y, core), tp: 4 (over x).
Axes of the slice: x: 4, y: 4, z: 4, core: 2. Of those that a mesh axis runs over, the one named last changes fastest.
Arguments:
- queries: bfloat16 [16384, 1024], P('sp', 'tp'), may hold values from -260 to 260, as said below
- keys: bfloat16 [16384, 512], P('sp', 'tp'), may hold values from -8 to 8, as said below
- values: bfloat16 [16384, 512], P('sp', 'tp'), may hold values from -24 to 24
- doc_ids: int32 [16384], P('sp'), may hold values from 0 to 7, never falling along the last dimension, each value on 1 to 8192 neighbouring positions
- sink_logit: float32 [8], P('tp'), may hold values from 2 to 7
- residual_in: bfloat16 [16384, 2048], P(('sp', 'tp')), may hold values from -6 to 6
- w_out: bfloat16 [1024, 2048], replicated, may hold values from -0.375 to 0.375
- gain_one: float32 [2048], replicated, may hold values from 0.1 to 1.9
- w_gate: bfloat16 [2048, 5632], P('sp', 'tp'), may hold values from -0.125 to 0.125
- w_up: bfloat16 [2048, 5632], P('sp', 'tp'), may hold values from -0.125 to 0.125
- w_down: bfloat16 [5632, 2048], P('tp', 'sp'), may hold values from -0.078125 to 0.078125
- gain_two: float32 [2048], replicated, may hold values from 0.1 to 1.9
Outputs:
- layer_out: bfloat16 [16384, 2048], P(('sp', 'tp'))
The draws below stay inside these ranges and needn't reach their ends.
Inputs may be any that keep to these rules, and one draw needn't show every extreme that they name: Real-valued projected queries. Real-valued projected keys. `doc_ids`: document numbers never fall along the sequence; each document is one run of positions.
All inputs are finite; a program needn't handle non-finite values.
Results may differ from the reference program's by a relative error of at most 0.012.
Values may be sent and summed in bfloat16 or wider, within the bound.
No kernel may reach another device: no remote copies, remote signals or barrier semaphores. Data moves between devices by JAX's collectives and lax.ppermute only.
A program may use at most 128 MiB of HBM per device.

```python
import math
import jax
import jax.numpy as jnp
import numpy as np
from jax import lax

D = 2048
QH = 8
HEAD = 128
FF = 5632
HALF = 128
SEQ = 16384
QW = 1024
KVW = 512
FF_DEV = 1408
N_SP = 32
N_TP = 4


def paired_draw(key):
    key = jax.random.fold_in(key, 11)
    first_key, second_key = jax.random.split(key, 2)
    keys_f = jnp.clip(jax.random.normal(first_key, (SEQ, KVW), jnp.float32), -7.5, 7.5)
    queries_f = jnp.clip(jax.random.normal(second_key, (SEQ, QW), jnp.float32), -7.5, 7.5)
    return (queries_f, keys_f)


def draw_queries(key, part):
    return paired_draw(key)[0].astype(jnp.bfloat16)


def draw_keys(key, part):
    return paired_draw(key)[1].astype(jnp.bfloat16)


def levels(rng, shape, cuts, least, high):
    level = 1.0
    for axis_at, parts in cuts:
        steps = jax.random.uniform(jax.random.fold_in(jax.random.fold_in(rng, 6), axis_at), (parts,), jnp.float32, least / len(cuts), high / len(cuts))
        level = level * jnp.repeat(jnp.exp(steps), shape[axis_at] // parts).reshape((-1,) + (1,) * (len(shape) - 1 - axis_at))
    return level


def length_profile(count, total, most, skew):
    weights = [(1 << 20) // math.isqrt(standing ** skew) + 1 for standing in range(2, count + 1)]
    rest, counts = total - most - (count - 1), [1] * (count - 1)
    while rest > 0:
        candidates = [i for i in range(count - 1) if counts[i] < most]
        mass, budget = sum([weights[i] for i in candidates]), rest
        for i in candidates:
            more = min(most - counts[i], max(1, budget * weights[i] // mass), rest)
            counts[i] = counts[i] + more
            rest = rest - more
    return np.array([most] + counts)


def ragged_sizes(key, count, total, most, skew):
    if count == 2:
        one = jax.random.randint(key, (), max(1, total - most), min(most, total - 1) + 1)
        return jnp.stack([one, total - one])
    sizes = jnp.asarray(length_profile(count, total, most, skew), jnp.int32)
    twos = (count - 1) // 2
    donor, receiver = sizes[1:1 + 2 * twos:2], sizes[2:2 + 2 * twos:2]
    margin = jnp.minimum(donor - 1, most - receiver)
    moved = jax.random.randint(jax.random.fold_in(key, 1), (twos,), 0, 1 << 20) % (margin + 1)
    sizes = sizes.at[1:1 + 2 * twos:2].set(donor - moved).at[2:2 + 2 * twos:2].set(receiver + moved)
    return sizes[jax.random.permutation(jax.random.fold_in(key, 2), count)]


def scatter_about(stream_key, shape, spread, limit, cuts=(), kind=jnp.bfloat16):
    array = jax.random.normal(stream_key, shape, jnp.float32) * spread
    if len(cuts) > 0:
        array = levels(stream_key, shape, cuts, -0.22, 0.18) * array
    return jnp.clip(array, min=-limit, max=limit).astype(kind)


def setup_inputs(seed: int = 0) -> dict:
    key_list = jax.random.split(jax.random.key(seed), 13)
    return {
        "queries": draw_queries(jax.random.fold_in(key_list[12], 71), 0),
        "keys": draw_keys(jax.random.fold_in(key_list[12], 71), 0),
        "values": scatter_about(key_list[2], (SEQ, KVW), 4.0, 24.0, ((0, 32), (1, 4))),
        "doc_ids": jnp.searchsorted(jnp.cumsum(ragged_sizes(key_list[3], max(N_SP // 4, 2), SEQ, SEQ // 2, 1)), jnp.arange(SEQ), side="right").astype(jnp.int32),
        "sink_logit": jnp.clip(2.0 + 5.0 * jax.random.uniform(key_list[4], (QH,), jnp.float32) ** levels(key_list[4], (QH,), ((0, 4),), -0.2, 0.2), 2.0, 7.0),
        "residual_in": scatter_about(key_list[5], (SEQ, D), 1.0, 6.0, ((0, 128),)),
        "w_out": scatter_about(key_list[6], (QW, D), (QW // 4) ** -0.5, 0.375),
        "gain_one": jnp.clip(1.0 + 0.18 * jax.random.normal(key_list[7], (D,), jnp.float32), 0.1, 1.9),
        "w_gate": scatter_about(key_list[8], (D, FF), D ** -0.5, 0.125, ((0, 32), (1, 4))),
        "w_up": scatter_about(key_list[9], (D, FF), D ** -0.5, 0.125, ((0, 32), (1, 4))),
        "w_down": scatter_about(key_list[10], (FF, D), FF ** -0.5, 0.078125, ((0, 4), (1, 32))),
        "gain_two": jnp.clip(1.0 + 0.18 * jax.random.normal(key_list[11], (D,), jnp.float32), 0.1, 1.9),
    }


ALPHA = 2.0 ** 0.5
EPS = 1e-05
NEGATIVE = -1e+30

def layer_norm(values_in, gain):
    average = lax.optimization_barrier(jnp.mean(values_in, -1, keepdims=True))
    centred = values_in - average
    variance = lax.optimization_barrier(jnp.mean(centred * centred, -1, keepdims=True))
    return centred * lax.rsqrt(variance + EPS) * gain

def attend(queries, keys, values, doc_ids, sink_logit):
    seq_len = queries.shape[0]
    kv_heads = keys.shape[1] // HEAD
    repeat = queries.shape[1] // keys.shape[1]
    block = math.gcd(512, seq_len)
    span = block + 2 * HALF
    keys_pad = jnp.pad(keys, ((HALF, HALF), (0, 0)))
    values_pad = jnp.pad(values, ((HALF, HALF), (0, 0)))
    docs_pad = jnp.pad(doc_ids, (HALF, HALF), constant_values=-1)
    sinks = sink_logit.reshape(kv_heads, repeat)

    def one_block(index):
        start = index * block
        query_blk = lax.dynamic_slice_in_dim(queries, start, block, 0).reshape(block, kv_heads, repeat, HEAD)
        key_blk = lax.dynamic_slice_in_dim(keys_pad, start, span, 0).reshape(span, kv_heads, HEAD)
        value_blk = lax.dynamic_slice_in_dim(values_pad, start, span, 0).reshape(span, kv_heads, HEAD)
        doc_query = lax.dynamic_slice_in_dim(doc_ids, start, block, 0)
        doc_key = lax.dynamic_slice_in_dim(docs_pad, start, span, 0)
        pos_query = start + jnp.arange(block, dtype=jnp.int32)
        pos_key = start - HALF + jnp.arange(span, dtype=jnp.int32)
        offset = pos_key[None, :] - pos_query[:, None]
        allowed = (jnp.abs(offset) <= HALF) & (doc_key[None, :] == doc_query[:, None])
        allowed = allowed & (pos_key[None, :] >= 0) & (pos_key[None, :] < seq_len)
        scores = jnp.einsum('qgrd,kgd->grqk', query_blk.astype(jnp.float32), key_blk.astype(jnp.float32)) * HEAD ** (-0.5)
        scores = jnp.where(allowed[None, None], scores, NEGATIVE)
        top = jnp.maximum(lax.optimization_barrier(jnp.max(scores, -1)), sinks[:, :, None])
        weights = jnp.exp(scores - top[..., None])
        total = lax.optimization_barrier(jnp.sum(weights, -1)) + jnp.exp(sinks[:, :, None] - top)
        weights = weights.astype(jnp.bfloat16)
        summed = jnp.einsum('grqk,kgd->qgrd', weights.astype(jnp.float32), value_blk.astype(jnp.float32))
        scaled = summed / jnp.transpose(total, (2, 0, 1))[..., None]
        return scaled.reshape(block, kv_heads * repeat * HEAD).astype(jnp.bfloat16)
    blocks = lax.map(one_block, jnp.arange(seq_len // block, dtype=jnp.int32))
    return blocks.reshape(seq_len, -1)

def reference(queries, keys, values, doc_ids, sink_logit, residual_in, w_out, gain_one, w_gate, w_up, w_down, gain_two):
    attended = attend(queries, keys, values, doc_ids, sink_logit)
    mixed = jnp.dot(attended, w_out, preferred_element_type=jnp.float32)
    pre_one = ALPHA * residual_in.astype(jnp.float32) + mixed
    normed = layer_norm(pre_one, gain_one).astype(jnp.bfloat16)
    gate_part = jnp.dot(normed, w_gate, preferred_element_type=jnp.float32)
    up_part = jnp.dot(normed, w_up, preferred_element_type=jnp.float32)
    hidden = (jax.nn.silu(gate_part) * up_part).astype(jnp.bfloat16)

    def partial_down(carry, index):
        hidden_blk = lax.dynamic_slice_in_dim(hidden, index * FF_DEV, FF_DEV, 1)
        weight_blk = lax.dynamic_slice_in_dim(w_down, index * FF_DEV, FF_DEV, 0)
        term = jnp.dot(hidden_blk, weight_blk, preferred_element_type=jnp.float32).astype(jnp.bfloat16)
        term = lax.optimization_barrier(term).astype(jnp.float32)
        return (carry + term, None)
    down, _ = lax.scan(partial_down, jnp.zeros((SEQ, D), jnp.float32), jnp.arange(N_TP, dtype=jnp.int32))
    pre_two = ALPHA * normed.astype(jnp.float32) + down
    return layer_norm(pre_two, gain_two).astype(jnp.bfloat16)
```

```python
import jax
import jax.numpy as jnp
from jax import lax
from jax.experimental import pallas as pl
from jax.experimental.pallas import tpu as pltpu
from jax.sharding import PartitionSpec as P


HEAD = 128
HALF = 128
ALPHA = 2.0**0.5
EPS = 1e-05
NEGATIVE = -1e30
BF, F32 = jnp.bfloat16, jnp.float32

ROWS = 512
OWN = 128
D = 2048
FFH = 704
GU = 2 * FFH
DN = 768
ORDER = (0, 1, 3, 2)
SP_Y, SP_Z = 2, 8


def swap(value, axis, mask):
    count = lax.axis_size(axis)
    return lax.ppermute(value, axis, [(i, i ^ mask) for i in range(count)])


def ring(value, axis, low):
    return [value] + [swap(value, axis, low * m) for m in ORDER[1:]]


def call(body, outs, flops, bytes_accessed, args, scratch=(), vmem_mib=20):
    vmem = pl.BlockSpec(memory_space=pltpu.VMEM)
    return pl.pallas_call(
        body,
        out_shape=outs,
        in_specs=[vmem] * len(args),
        out_specs=jax.tree.map(lambda _: vmem, outs),
        scratch_shapes=list(scratch),
        compiler_params=pltpu.CompilerParams(vmem_limit_bytes=vmem_mib << 20),
        cost_estimate=pl.CostEstimate(
            flops=flops, bytes_accessed=bytes_accessed, transcendentals=0
        ),
    )(*args)


def shape(dims, dtype=BF):
    return jax.ShapeDtypeStruct(dims, dtype)


def pack_body(gate, up, down, keep, send):
    core = lax.axis_index("sp") % 2
    lane = lax.broadcasted_iota(jnp.int32, (64, GU), 1)
    low = lane < FFH
    g, u, d = (r[...].astype(F32) for r in (gate, up, down))
    gr, ur, dr = (pltpu.roll(v, FFH, 1) for v in (g, u, d))
    first = jnp.where(low, g, ur)
    second = jnp.where(low, gr, u)
    d0 = jnp.where(low, d, 0.0)[:, :DN]
    d1 = jnp.where(low, dr, 0.0)[:, :DN]
    zero = core == 0
    keep[:, :GU] = jnp.where(zero, first, second).astype(BF)
    keep[:, GU:] = jnp.where(zero, d0, d1).astype(BF)
    send[:, :GU] = jnp.where(zero, second, first).astype(BF)
    send[:, GU:] = jnp.where(zero, d1, d0).astype(BF)


def attend_body(q, k, v, docs, sinks, side, far, out, kv, drow):
    sp = lax.axis_index("sp")
    core = sp % 2
    zero = core == 0
    before = jnp.where(zero, far[...].astype(F32), side[...].astype(F32))
    after = jnp.where(zero, side[...].astype(F32), far[...].astype(F32))
    kv[0:HALF, :] = before[:HALF].astype(BF)
    kv[HALF : HALF + ROWS, :HEAD] = k[...]
    kv[HALF : HALF + ROWS, HEAD:] = v[...]
    kv[HALF + ROWS :, :] = after[:HALF].astype(BF)
    drow[:, 0:HALF] = jnp.where(sp == 0, -1.0, before[HALF:, :HALF])
    drow[:, HALF : HALF + ROWS] = jnp.broadcast_to(docs[...].astype(F32), (8, ROWS))
    drow[:, HALF + ROWS :] = jnp.where(
        sp == lax.axis_size("sp") - 1, -1.0, after[HALF:, :HALF]
    )
    span = 3 * HALF
    row = lax.broadcasted_iota(jnp.int32, (HALF, span), 0)
    col = lax.broadcasted_iota(jnp.int32, (HALF, span), 1)
    near = jnp.abs(col - HALF - row) <= HALF
    for b in range(ROWS // HALF):
        dq = jnp.broadcast_to(drow[0:1, HALF + b * HALF : 2 * HALF + b * HALF], (HALF, HALF)).T
        dk = drow[0:1, b * HALF : b * HALF + span]
        same = jnp.concatenate([dq, dq, dq], 1) == dk
        ok = near & same
        keys = kv[b * HALF : b * HALF + span, :HEAD]
        vals = kv[b * HALF : b * HALF + span, HEAD:]
        for h in range(2):
            rows = slice(b * HALF, (b + 1) * HALF)
            cols = slice(h * HEAD, (h + 1) * HEAD)
            s = lax.dot_general(
                q[rows, cols], keys, (((1,), (1,)), ((), ())), preferred_element_type=F32
            ) * HEAD ** (-0.5)
            s = jnp.where(ok, s, NEGATIVE)
            sink = sinks[0:1, h : h + 1]
            top = jnp.maximum(jnp.max(s, -1, keepdims=True), sink)
            w = jnp.exp(s - top)
            total = jnp.sum(w, -1, keepdims=True) + jnp.exp(sink - top)
            o = jnp.dot(w.astype(BF), vals, preferred_element_type=F32)
            out[rows, cols] = (o / total).astype(BF)


def normalised(value):
    average = jnp.mean(value, -1, keepdims=True)
    centred = value - average
    variance = jnp.mean(centred * centred, -1, keepdims=True)
    return centred * lax.rsqrt(variance + EPS)


def chip(rz, ry):
    sp = lax.axis_index("sp")
    y, z = (sp // SP_Y) % 4, sp // SP_Z
    return pl.multiple_of(((z ^ rz) * 4 + (y ^ ry)) * 128, 128)


def norm_body(a0, a1, a3, a2, w_out, r0, r1, r3, r2, gain, out, mixed, nat, rot):
    x = lax.axis_index("tp")
    atts, res = (a0, a1, a3, a2), (r0, r1, r3, r2)
    for n in range(0, D, 512):
        acc = None
        for mask, a in zip(ORDER, atts):
            w = w_out[pl.ds(pl.multiple_of((x ^ mask) * 256, 256), 256), n : n + 512]
            t = jnp.dot(a[...], w, preferred_element_type=F32)
            acc = t if acc is None else acc + t
        mixed[:, n : n + 512] = acc
    for mask, r in zip(ORDER, res):
        for s in range(0, OWN, 32):
            at = pl.ds(pl.multiple_of((x ^ mask) * OWN + s, 32), 32)
            v = mixed[at, :] + ALPHA * r[s : s + 32, :].astype(F32)
            n = normalised(v) * gain[...]
            nat[at, :] = n
    for t in range(0, D, 128):
        rot[:, t : t + 128] = pltpu.roll(nat[:, t : t + 128], 64, 1)
    low = lax.broadcasted_iota(jnp.int32, (ROWS, 128), 1) < 64
    for i in range(4):
        for j in (0, 2):
            a, b = (pl.ds(chip(ORDER[i], ORDER[k]), 128) for k in (j, j + 1))
            dst = (i * 4 + j) * 64
            out[:, dst : dst + 128] = jnp.where(low, nat[:, a], rot[:, b]).astype(BF)
            a, b = (pl.ds(chip(ORDER[k], ORDER[i]), 128) for k in (j, j + 1))
            dst += 1024
            out[:, dst : dst + 128] = jnp.where(low, rot[:, a], nat[:, b]).astype(BF)


def hidden_body(mine, other, *refs):
    pieces, out, acc = refs[:10], refs[10], refs[11]
    for half, src in enumerate((mine, other)):
        for n in range(0, GU, 256):
            m = min(n + 256, GU)
            w = jnp.concatenate([p[:, n:m] for p in pieces], 0)
            acc[:, n:m] = jnp.dot(src[...], w, preferred_element_type=F32)
        for s in range(0, ROWS, 64):
            v = acc[s : s + 64, :]
            up = pltpu.roll(v, FFH, 1)[:, :DN]
            gate = v[:, :DN]
            h = gate / (1.0 + jnp.exp(-gate)) * up
            live = lax.broadcasted_iota(jnp.int32, (64, DN), 1) < FFH
            out[half * ROWS + s : half * ROWS + s + 64, :] = jnp.where(live, h, 0.0).astype(BF)


def down_part(h, p):
    return lax.dot_general(h, p, (((1,), (1,)), ((), ())), preferred_element_type=F32)


def give_body(h, *refs):
    pieces, out = refs[:-1], refs[-1]
    at = 0
    for p in pieces:
        width = p.shape[0]
        out[:, at : at + width] = down_part(h[ROWS:, :], p[...]).astype(BF)
        at += width


def take_body(h, theirs, *refs):
    pieces, (s0, s1, s3, s2, own) = refs[:-5], refs[-5:]
    x = lax.axis_index("tp")
    at = 0
    for p in pieces:
        width = p.shape[0]
        cols = slice(at, at + width)
        own[:, cols] = down_part(h[:ROWS, :], p[...]) + theirs[:, cols].astype(F32)
        at += width
    for mask, dst in zip(ORDER, (s0, s1, s3, s2)):
        rows = pl.ds(pl.multiple_of((x ^ mask) * OWN, OWN), OWN)
        dst[...] = own[rows, :].astype(dst.dtype)


def final_body(normed, gain, *refs):
    parts, out, pre = refs[:12], refs[12], refs[13]
    x = lax.axis_index("tp")
    xs = pl.ds(pl.multiple_of(x * OWN, OWN), OWN)
    for c, (first, width) in enumerate(((0, 256), (256, 512), (768, 256))):
        s = [r for r in parts[4 * c : 4 * c + 4]]
        v = s[0][...] + s[1][...].astype(F32) + s[2][...].astype(F32) + s[3][...].astype(F32)
        for kind in range(2):
            dst = slice(kind * 1024 + first, kind * 1024 + first + width)
            n = normed[xs, dst].astype(F32)
            pre[:, dst] = ALPHA * n + v[:, kind * width : (kind + 1) * width]
    pre[...] = normalised(pre[...])
    low = lax.broadcasted_iota(jnp.int32, (OWN, 128), 1) < 64
    for i in range(4):
        for j in range(4):
            p, q = 4 * i + j, 4 * j + i
            a = pre[:, (p // 2) * 128 : (p // 2) * 128 + 128]
            b = pre[:, 1024 + (q // 2) * 128 : 1024 + (q // 2) * 128 + 128]
            if p % 2 == 1:
                a = pltpu.roll(a, 64, 1)
            if q % 2 == 0:
                b = pltpu.roll(b, 64, 1)
            at = pl.ds(chip(ORDER[i], ORDER[j]), 128)
            out[:, at] = (jnp.where(low, a, b) * gain[:, at]).astype(BF)


def spread(col, low):
    one = swap(col, "sp", low)
    three = swap(col, "sp", 3 * low)
    mid = col.shape[0] // 2
    two_a = swap(one[:mid], "sp", 3 * low)
    two_b = swap(three[mid:], "sp", low)
    return col, one, three, two_a, two_b


def per_device(
    queries,
    keys,
    values,
    doc_ids,
    sink_logit,
    residual_in,
    w_out,
    gain_one,
    w_gate,
    w_up,
    w_down,
    gain_two,
):
    core = lax.axis_index("sp") % 2
    keep, send = call(
        pack_body, (shape((64, GU + DN)),) * 2, 10**6, 10**6, (w_gate, w_up, w_down.T)
    )
    recv = swap(send, "sp", 1)
    from_0 = jnp.where(core == 0, keep, recv)
    from_1 = jnp.where(core == 0, recv, keep)

    docs8 = jnp.broadcast_to(doc_ids.astype(BF).reshape(1, ROWS), (8, ROWS))

    def edge(rows):
        kv = jnp.concatenate([keys[rows], values[rows]], 1)
        d = docs8[:, rows]
        return jnp.concatenate([kv, jnp.concatenate([d, d], 1)], 0)

    last, first = edge(slice(ROWS - HALF, ROWS)), edge(slice(0, HALF))
    side = swap(jnp.where(core == 0, last, first), "sp", 1)
    count = lax.axis_size("sp")
    pairs = [(i, i + 1) for i in range(1, count - 1, 2)]
    far = lax.ppermute(
        jnp.where(core == 0, first, last), "sp", pairs + [(b, a) for a, b in pairs]
    )

    res = ring(residual_in, "tp", 1)

    def columns(origin, near, across):
        units = ring(origin, "sp", near)
        gu = jnp.concatenate([u[:, :GU] for u in units], 0)
        dn = jnp.concatenate([u[:, GU:] for u in units], 0)
        return spread(gu, across), ring(dn, "sp", across)

    gu_a, dn_a = columns(from_0, SP_Y, SP_Z)
    gu_b, dn_b = columns(from_1, SP_Z, SP_Y)

    attended = call(
        attend_body,
        shape((ROWS, 256)),
        4 * ROWS * 256 * 384 * 8,
        10**6,
        (queries, keys, values, doc_ids.reshape(1, ROWS), sink_logit.reshape(1, 2), side, far),
        (pltpu.VMEM((ROWS + 2 * HALF, 256), BF), pltpu.VMEM((8, ROWS + 2 * HALF), F32)),
    )
    atts = ring(attended, "tp", 1)
    mine = call(
        norm_body,
        shape((ROWS, D)),
        2 * ROWS * 1024 * D * 2,
        10**7,
        (*atts, w_out, *res, gain_one.reshape(1, D)),
        (pltpu.VMEM((ROWS, D), F32),) * 3,
    )
    other = swap(mine, "sp", 1)
    hidden = call(
        hidden_body,
        shape((2 * ROWS, DN)),
        2 * 2 * ROWS * D * GU,
        10**7,
        (mine, other, *gu_a, *gu_b),
        (pltpu.VMEM((ROWS, GU), F32),),
    )
    sums = []
    chunks = [slice(0, 1), slice(1, 3), slice(3, 4)]
    for part_of in chunks:
        pieces = (*dn_a[part_of], *dn_b[part_of])
        width = sum(p.shape[0] for p in pieces)
        flops = 2 * ROWS * DN * width
        part = call(give_body, shape((ROWS, width)), flops, 10**6, (hidden, *pieces))
        theirs = swap(part, "sp", 1)
        s0, *rest = call(
            take_body,
            (shape((OWN, width), F32),) + (shape((OWN, width)),) * 3,
            flops,
            10**6,
            (hidden, theirs, *pieces),
            (pltpu.VMEM((ROWS, width), F32),),
        )
        sums += [s0] + [swap(r, "tp", m) for r, m in zip(rest, ORDER[1:])]
    return call(
        final_body,
        shape((OWN, D)),
        10**6,
        10**6,
        (mine, gain_two.reshape(1, D), *sums),
        (pltpu.VMEM((OWN, D), F32),),
    )


def solution(mesh):
    in_specs = (
        P("sp", "tp"),
        P("sp", "tp"),
        P("sp", "tp"),
        P("sp"),
        P("tp"),
        P(("sp", "tp"), None),
        P(),
        P(),
        P("sp", "tp"),
        P("sp", "tp"),
        P("tp", "sp"),
        P(),
    )
    out_specs = P(("sp", "tp"), None)
    return jax.shard_map(
        per_device, mesh=mesh, in_specs=in_specs, out_specs=out_specs, check_vma=False
    )
```

```python
import jax
import jax.numpy as jnp
from jax import lax
from jax.experimental import pallas as pl
from jax.experimental.pallas import tpu as pltpu
from jax.sharding import PartitionSpec as P


HEAD = 128
HALF = 128
ALPHA = 2.0**0.5
EPS = 1e-05
NEGATIVE = -1e30
BF, F32 = jnp.bfloat16, jnp.float32

ROWS = 512
OWN = 128
D = 2048
FFH = 704
GU = 2 * FFH
DN = 768
ORDER = (0, 1, 3, 2)
SP_Y, SP_Z = 2, 8


def swap(value, axis, mask):
    count = lax.axis_size(axis)
    return lax.ppermute(value, axis, [(i, i ^ mask) for i in range(count)])


def ring(value, axis, low):
    return [value] + [swap(value, axis, low * m) for m in ORDER[1:]]


def call(body, outs, flops, bytes_accessed, args, scratch=(), space=pltpu.VMEM, vmem_mib=20):
    vmem = pl.BlockSpec(memory_space=pltpu.VMEM)
    return pl.pallas_call(
        body,
        out_shape=outs,
        in_specs=[pl.BlockSpec(memory_space=space)] * len(args),
        out_specs=jax.tree.map(lambda _: vmem, outs),
        scratch_shapes=list(scratch),
        compiler_params=pltpu.CompilerParams(vmem_limit_bytes=vmem_mib << 20),
        cost_estimate=pl.CostEstimate(
            flops=flops, bytes_accessed=bytes_accessed, transcendentals=0
        ),
    )(*args)


def shape(dims, dtype=BF):
    return jax.ShapeDtypeStruct(dims, dtype)


def pack_body(
    gate, up, down, q, k, v, docs, sinks, *refs
):
    keep, send, side, far, q_o, k_o, v_o, docs_o, sinks_o, gate_v, up_v, down_v, sems = refs
    moves = [(gate, gate_v), (up, up_v), (down, down_v), (k, k_o), (v, v_o), (docs, docs_o)]
    moves += [(q, q_o), (sinks, sinks_o)]
    copies = [pltpu.make_async_copy(*m, sems.at[i]) for i, m in enumerate(moves)]
    for copy in copies:
        copy.start()
    zero = lax.axis_index("sp") % 2 == 0
    low = lax.broadcasted_iota(jnp.int32, (64, GU), 1) < FFH
    for copy in copies[:2]:
        copy.wait()
    g, u = gate_v[...].astype(F32), up_v[...].astype(F32)
    first = jnp.where(low, g, pltpu.roll(u, FFH, 1))
    second = jnp.where(low, pltpu.roll(g, FFH, 1), u)
    keep[:, :GU] = jnp.where(zero, first, second).astype(BF)
    send[:, :GU] = jnp.where(zero, second, first).astype(BF)
    copies[2].wait()
    d = down_v[...].astype(F32)
    d0 = jnp.where(low, d, 0.0)[:, :DN]
    d1 = jnp.where(low, pltpu.roll(d, FFH, 1), 0.0)[:, :DN]
    keep[:, GU:] = jnp.where(zero, d0, d1).astype(BF)
    send[:, GU:] = jnp.where(zero, d1, d0).astype(BF)
    for copy in copies[3:]:
        copy.wait()
    a, b = slice(0, HALF), slice(ROWS - HALF, ROWS)
    for out, end in ((side, zero), (far, jnp.logical_not(zero))):
        out[:HALF, :HEAD] = jnp.where(end, k_o[b, :], k_o[a, :])
        out[:HALF, HEAD:] = jnp.where(end, v_o[b, :], v_o[a, :])
        d = docs_o[...].astype(F32)
        d = jnp.where(end, d[:, b], d[:, a]).astype(BF)
        d = jnp.broadcast_to(d, (8, HALF))
        out[HALF:, :HEAD] = d
        out[HALF:, HEAD:] = d


def attend_body(q, k, v, docs, sinks, side, far, o0, o1, o3, o2, kv, drow):
    sp = lax.axis_index("sp")
    core = sp % 2
    zero = core == 0
    before = jnp.where(zero, far[...].astype(F32), side[...].astype(F32))
    after = jnp.where(zero, side[...].astype(F32), far[...].astype(F32))
    kv[0:HALF, :] = before[:HALF].astype(BF)
    kv[HALF : HALF + ROWS, :HEAD] = k[...]
    kv[HALF : HALF + ROWS, HEAD:] = v[...]
    kv[HALF + ROWS :, :] = after[:HALF].astype(BF)
    drow[:, 0:HALF] = jnp.where(sp == 0, -1.0, before[HALF:, :HALF])
    drow[:, HALF : HALF + ROWS] = jnp.broadcast_to(docs[...].astype(F32), (8, ROWS))
    drow[:, HALF + ROWS :] = jnp.where(
        sp == lax.axis_size("sp") - 1, -1.0, after[HALF:, :HALF]
    )
    span = 3 * HALF
    row = lax.broadcasted_iota(jnp.int32, (HALF, span), 0)
    col = lax.broadcasted_iota(jnp.int32, (HALF, span), 1)
    near = jnp.abs(col - HALF - row) <= HALF
    for mask, out in zip(ORDER, (o0, o1, o3, o2)):
        start = pl.multiple_of((lax.axis_index("tp") ^ mask) * HALF, HALF)
        own = pl.ds(pl.multiple_of(start + HALF, HALF), HALF)
        window = pl.ds(start, span)
        dq = jnp.broadcast_to(drow[0:1, own], (HALF, HALF)).T
        same = jnp.concatenate([dq, dq, dq], 1) == drow[0:1, window]
        ok = near & same
        keys = kv[window, :HEAD]
        vals = kv[window, HEAD:]
        for h in range(2):
            cols = slice(h * HEAD, (h + 1) * HEAD)
            s = lax.dot_general(
                q[pl.ds(start, HALF), cols],
                keys,
                (((1,), (1,)), ((), ())),
                preferred_element_type=F32,
            ) * HEAD ** (-0.5)
            s = jnp.where(ok, s, NEGATIVE)
            sink = sinks[0:1, h : h + 1]
            top = jnp.maximum(jnp.max(s, -1, keepdims=True), sink)
            w = jnp.exp(s - top)
            total = jnp.sum(w, -1, keepdims=True) + jnp.exp(sink - top)
            o = jnp.dot(w.astype(BF), vals, preferred_element_type=F32)
            out[:, cols] = (o / total).astype(BF)


def normalised(value):
    average = jnp.mean(value, -1, keepdims=True)
    centred = value - average
    variance = jnp.mean(centred * centred, -1, keepdims=True)
    return centred * lax.rsqrt(variance + EPS)


def chip(rz, ry):
    sp = lax.axis_index("sp")
    y, z = (sp // SP_Y) % 4, sp // SP_Z
    return pl.multiple_of(((z ^ rz) * 4 + (y ^ ry)) * 128, 128)


def norm_body(a0, a1, a3, a2, w_out, res, gain, out, nat, rot):
    x = lax.axis_index("tp")
    for n in range(0, D, 256):
        acc = ALPHA * res[:, n : n + 256].astype(F32)
        for mask, a in zip(ORDER, (a0, a1, a3, a2)):
            w = w_out[pl.ds(pl.multiple_of((x ^ mask) * 256, 256), 256), n : n + 256]
            acc = acc + jnp.dot(a[...], w, preferred_element_type=F32)
        nat[:, n : n + 256] = acc
    for s in range(0, OWN, 32):
        nat[s : s + 32, :] = normalised(nat[s : s + 32, :]) * gain[...]
    for t in range(0, D, 128):
        rot[:, t : t + 128] = pltpu.roll(nat[:, t : t + 128], 64, 1)
    low = lax.broadcasted_iota(jnp.int32, (OWN, 128), 1) < 64
    for i in range(4):
        for j in (0, 2):
            a, b = (pl.ds(chip(ORDER[i], ORDER[k]), 128) for k in (j, j + 1))
            dst = (i * 4 + j) * 64
            out[:, dst : dst + 128] = jnp.where(low, nat[:, a], rot[:, b]).astype(BF)
            a, b = (pl.ds(chip(ORDER[k], ORDER[i]), 128) for k in (j, j + 1))
            dst += 1024
            out[:, dst : dst + 128] = jnp.where(low, rot[:, a], nat[:, b]).astype(BF)


def product(rows, pieces, spans, acc, store):
    lhs = jnp.concatenate(
        [jnp.concatenate([r[:, a:b] for r in rows], 0) for a, b in spans], 1
    )
    for n in range(0, GU, 256):
        m = min(n + 256, GU)
        w = jnp.concatenate([p[:, n:m] for p in pieces], 0)
        t = jnp.dot(lhs, w, preferred_element_type=F32)
        store[:, n:m] = t if acc is None else acc[:, n:m] + t


def early_body(*refs):
    product(refs[:5], refs[5:17], ((0, 768), (1024, 1792)), None, refs[17])


def hidden_body(*refs):
    rows, pieces, early, out, acc = refs[:5], refs[5:9], refs[9], refs[10], refs[11]
    product(rows, pieces, ((768, 1024), (1792, 2048)), early, acc)
    live = lax.broadcasted_iota(jnp.int32, (64, DN), 1) < FFH
    for s in range(0, ROWS, 64):
        v = acc[s : s + 64, :]
        up = pltpu.roll(v, FFH, 1)[:, :DN]
        gate = v[:, :DN]
        h = gate / (1.0 + jnp.exp(-gate)) * up
        out[s : s + 64, :] = jnp.where(live, h, 0.0).astype(BF)


def down_parts(h, pieces):
    for i in range(0, len(pieces), 2):
        p = jnp.concatenate([r[:, GU:] for r in pieces[i : i + 2]], 0)
        at = i * 128
        yield (
            at,
            at + 256,
            lax.dot_general(h[...], p, (((1,), (1,)), ((), ())), preferred_element_type=F32),
        )


def give_body(h, *refs):
    pieces, out = refs[:-1], refs[-1]
    for a, b, v in down_parts(h, pieces):
        out[:, a:b] = v.astype(BF)


def take_body(h, theirs, *refs):
    pieces, (own, left, right, left_keep, right_keep) = refs[:-5], refs[-5:]
    half = own.shape[1] // 2
    for at, end, v in down_parts(h, pieces):
        v = v + theirs[:, at:end].astype(F32)
        b0, b1, b3, b2 = (v[k * OWN : (k + 1) * OWN, :] for k in range(4))
        own[:, at:end] = b0
        send, keep, near, away = (
            (left, left_keep, b1, b3) if at < half else (right, right_keep, b3, b1)
        )
        cols = slice(at % half, at % half + end - at)
        send[:OWN, cols] = near.astype(BF)
        send[OWN:, cols] = b2.astype(BF)
        keep[:, cols] = away


def fold_body(own, left, right, left_keep, right_keep, total, left_out, right_out):
    half = own.shape[1] // 2
    total[:, :half] = own[:, :half] + left[:OWN, :].astype(F32)
    total[:, half:] = own[:, half:] + right[:OWN, :].astype(F32)
    left_out[...] = (left_keep[...] + left[OWN:, :].astype(F32)).astype(BF)
    right_out[...] = (right_keep[...] + right[OWN:, :].astype(F32)).astype(BF)


def final_body(normed, gain, *refs):
    parts, out, pre = refs[:6], refs[6], refs[7]
    for c, (first, width) in enumerate(((0, 512), (512, 512))):
        total, *last = parts[3 * c : 3 * c + 3]
        for kind in range(2):
            dst = slice(kind * 1024 + first, kind * 1024 + first + width)
            n = normed[:, dst].astype(F32)
            v = total[:, kind * width : (kind + 1) * width] + last[kind][...].astype(F32)
            pre[:, dst] = ALPHA * n + v
    pre[...] = normalised(pre[...])
    low = lax.broadcasted_iota(jnp.int32, (OWN, 128), 1) < 64
    for i in range(4):
        for j in range(4):
            p, q = 4 * i + j, 4 * j + i
            a = pre[:, (p // 2) * 128 : (p // 2) * 128 + 128]
            b = pre[:, 1024 + (q // 2) * 128 : 1024 + (q // 2) * 128 + 128]
            if p % 2 == 1:
                a = pltpu.roll(a, 64, 1)
            if q % 2 == 0:
                b = pltpu.roll(b, 64, 1)
            at = pl.ds(chip(ORDER[i], ORDER[j]), 128)
            out[:, at] = (jnp.where(low, a, b) * gain[:, at]).astype(BF)


def spread(low_half, high_half, axis, low):
    one = swap(low_half, axis, low), swap(high_half, axis, low)
    three = swap(low_half, axis, 3 * low), swap(high_half, axis, 3 * low)
    two = swap(one[0], axis, 3 * low), swap(three[1], axis, low)
    return (low_half, high_half, *one, *three, *two)


def per_device(
    queries,
    keys,
    values,
    doc_ids,
    sink_logit,
    residual_in,
    w_out,
    gain_one,
    w_gate,
    w_up,
    w_down,
    gain_two,
):
    core = lax.axis_index("sp") % 2
    local = (queries, keys, values, doc_ids.reshape(1, ROWS), sink_logit.reshape(1, 2))
    keep, send, inner, outer, *local = call(
        pack_body,
        (shape((64, GU + DN)),) * 2
        + (shape((HALF + 8, 2 * HEAD)),) * 2
        + tuple(shape(a.shape, a.dtype) for a in local),
        10**6,
        10**6,
        tuple(
            pltpu.with_memory_space_constraint(a, pltpu.HBM)
            for a in (w_gate, w_up, w_down.T, *local)
        ),
        [pltpu.VMEM((64, GU), BF)] * 3 + [pltpu.SemaphoreType.DMA((8,))],
        pltpu.HBM,
    )
    recv = swap(send, "sp", 1)
    from_0 = jnp.where(core == 0, keep, recv)
    from_1 = jnp.where(core == 0, recv, keep)

    side = swap(inner, "sp", 1)
    count = lax.axis_size("sp")
    pairs = [(i, i + 1) for i in range(1, count - 1, 2)]
    far = lax.ppermute(outer, "sp", pairs + [(b, a) for a, b in pairs])

    def columns(origin, near, across):
        units = ring(origin, "sp", near)
        halves = (jnp.concatenate(units[i : i + 2], 0) for i in (0, 2))
        return spread(*halves, "sp", across)

    all_a = columns(from_0, SP_Y, SP_Z)
    all_b = columns(from_1, SP_Z, SP_Y)

    attended = call(
        attend_body,
        (shape((OWN, 256)),) * 4,
        4 * ROWS * 256 * 384 * 8,
        10**6,
        (*local, side, far),
        (pltpu.VMEM((ROWS + 2 * HALF, 256), BF), pltpu.VMEM((8, ROWS + 2 * HALF), F32)),
    )
    atts = [swap(a, "tp", m) if m else a for m, a in zip(ORDER, attended)]
    normed = call(
        norm_body,
        shape((OWN, D)),
        2 * OWN * 1024 * D * 4,
        10**7,
        (*atts, w_out, residual_in, gain_one.reshape(1, D)),
        (pltpu.VMEM((OWN, D), F32),) * 2,
    )
    x1, x3 = swap(normed, "tp", 1), swap(normed, "tp", 3)
    mid = OWN // 2
    rows = (normed, x1, x3, swap(x1[:mid], "tp", 3), swap(x3[mid:], "tp", 1))
    others = [swap(r, "sp", 1) for r in rows]

    def hidden_of(r):
        early = call(
            early_body,
            shape((ROWS, GU), F32),
            2 * ROWS * 1536 * GU,
            10**7,
            (*r, *all_a[:6], *all_b[:6]),
        )
        return call(
            hidden_body,
            shape((ROWS, DN)),
            2 * ROWS * 512 * GU,
            10**7,
            (*r, *all_a[6:], *all_b[6:], early),
            (pltpu.VMEM((ROWS, GU), F32),),
        )

    own_hidden, other_hidden = hidden_of(rows), hidden_of(others)
    sums = []
    chunks = [slice(0, 4), slice(4, 8)]
    for part_of in chunks:
        pieces = (*all_a[part_of], *all_b[part_of])
        width = sum(p.shape[0] for p in pieces)
        flops = 2 * ROWS * DN * width
        part = call(give_body, shape((ROWS, width)), flops, 10**6, (other_hidden, *pieces))
        theirs = swap(part, "sp", 1)
        half = width // 2
        own, left, right, *keeps = call(
            take_body,
            (shape((OWN, width), F32),)
            + (shape((2 * OWN, half)),) * 2
            + (shape((OWN, half), F32),) * 2,
            flops,
            10**6,
            (own_hidden, theirs, *pieces),
        )
        left, right = swap(left, "tp", 1), swap(right, "tp", 3)
        own, left, right = call(
            fold_body,
            (shape((OWN, width), F32),) + (shape((OWN, half)),) * 2,
            10**6,
            10**6,
            (own, left, right, *keeps),
        )
        sums += [own, swap(left, "tp", 3), swap(right, "tp", 1)]
    return call(
        final_body,
        shape((OWN, D)),
        10**6,
        10**6,
        (normed, gain_two.reshape(1, D), *sums),
        (pltpu.VMEM((OWN, D), F32),),
    )


def solution(mesh):
    in_specs = (
        P("sp", "tp"),
        P("sp", "tp"),
        P("sp", "tp"),
        P("sp"),
        P("tp"),
        P(("sp", "tp"), None),
        P(),
        P(),
        P("sp", "tp"),
        P("sp", "tp"),
        P("tp", "sp"),
        P(),
    )
    out_specs = P(("sp", "tp"), None)
    return jax.shard_map(
        per_device, mesh=mesh, in_specs=in_specs, out_specs=out_specs, check_vma=False
    )
```

```python
import jax
import jax.numpy as jnp
from jax import lax
from jax.experimental import pallas as pl
from jax.experimental.pallas import tpu as pltpu
from jax.sharding import PartitionSpec as P


HEAD = 128
HALF = 128
ALPHA = 2.0**0.5
EPS = 1e-05
NEGATIVE = -1e30
BF, F32 = jnp.bfloat16, jnp.float32

ROWS = 512
OWN = 128
D = 2048
FFH = 704
GU = 2 * FFH
DN = 768
ORDER = (0, 1, 3, 2)
SP_Y, SP_Z = 2, 8


def swap(value, axis, mask):
    count = lax.axis_size(axis)
    return lax.ppermute(value, axis, [(i, i ^ mask) for i in range(count)])


def ring(value, axis, low):
    return [value] + [swap(value, axis, low * m) for m in ORDER[1:]]


def call(body, outs, flops, bytes_accessed, args, scratch=(), space=pltpu.VMEM, vmem_mib=20):
    vmem = pl.BlockSpec(memory_space=pltpu.VMEM)
    return pl.pallas_call(
        body,
        out_shape=outs,
        in_specs=[pl.BlockSpec(memory_space=space)] * len(args),
        out_specs=jax.tree.map(lambda _: vmem, outs),
        scratch_shapes=list(scratch),
        compiler_params=pltpu.CompilerParams(vmem_limit_bytes=vmem_mib << 20),
        cost_estimate=pl.CostEstimate(
            flops=flops, bytes_accessed=bytes_accessed, transcendentals=0
        ),
    )(*args)


def shape(dims, dtype=BF):
    return jax.ShapeDtypeStruct(dims, dtype)


def pack_body(
    gate, up, down, q, k, v, docs, sinks, *refs
):
    keep, send, side, far, q_o, k_o, v_o, docs_o, sinks_o, gate_v, up_v, down_v, sems = refs
    moves = [(gate, gate_v), (up, up_v), (down, down_v), (k, k_o), (v, v_o), (docs, docs_o)]
    moves += [(q, q_o), (sinks, sinks_o)]
    copies = [pltpu.make_async_copy(*m, sems.at[i]) for i, m in enumerate(moves)]
    for copy in copies:
        copy.start()
    zero = lax.axis_index("sp") % 2 == 0
    low = lax.broadcasted_iota(jnp.int32, (64, GU), 1) < FFH
    for copy in copies[:2]:
        copy.wait()
    g, u = gate_v[...].astype(F32), up_v[...].astype(F32)
    first = jnp.where(low, g, pltpu.roll(u, FFH, 1))
    second = jnp.where(low, pltpu.roll(g, FFH, 1), u)
    keep[:, :GU] = jnp.where(zero, first, second).astype(BF)
    send[:, :GU] = jnp.where(zero, second, first).astype(BF)
    copies[2].wait()
    d = down_v[...].astype(F32)
    d0 = jnp.where(low, d, 0.0)[:, :DN]
    d1 = jnp.where(low, pltpu.roll(d, FFH, 1), 0.0)[:, :DN]
    keep[:, GU:] = jnp.where(zero, d0, d1).astype(BF)
    send[:, GU:] = jnp.where(zero, d1, d0).astype(BF)
    for copy in copies[3:]:
        copy.wait()
    a, b = slice(0, HALF), slice(ROWS - HALF, ROWS)
    for out, end in ((side, zero), (far, jnp.logical_not(zero))):
        out[:HALF, :HEAD] = jnp.where(end, k_o[b, :], k_o[a, :])
        out[:HALF, HEAD:] = jnp.where(end, v_o[b, :], v_o[a, :])
        d = docs_o[...].astype(F32)
        d = jnp.where(end, d[:, b], d[:, a]).astype(BF)
        d = jnp.broadcast_to(d, (8, HALF))
        out[HALF:, :HEAD] = d
        out[HALF:, HEAD:] = d


def attend_body(q, k, v, docs, sinks, side, far, o0, o1, o3, o2, kv, drow):
    sp = lax.axis_index("sp")
    core = sp % 2
    zero = core == 0
    before = jnp.where(zero, far[...].astype(F32), side[...].astype(F32))
    after = jnp.where(zero, side[...].astype(F32), far[...].astype(F32))
    kv[0:HALF, :] = before[:HALF].astype(BF)
    kv[HALF : HALF + ROWS, :HEAD] = k[...]
    kv[HALF : HALF + ROWS, HEAD:] = v[...]
    kv[HALF + ROWS :, :] = after[:HALF].astype(BF)
    drow[:, 0:HALF] = jnp.where(sp == 0, -1.0, before[HALF:, :HALF])
    drow[:, HALF : HALF + ROWS] = jnp.broadcast_to(docs[...].astype(F32), (8, ROWS))
    drow[:, HALF + ROWS :] = jnp.where(
        sp == lax.axis_size("sp") - 1, -1.0, after[HALF:, :HALF]
    )
    span = 3 * HALF
    row = lax.broadcasted_iota(jnp.int32, (HALF, span), 0)
    col = lax.broadcasted_iota(jnp.int32, (HALF, span), 1)
    near = jnp.abs(col - HALF - row) <= HALF
    for mask, out in zip(ORDER, (o0, o1, o3, o2)):
        start = pl.multiple_of((lax.axis_index("tp") ^ mask) * HALF, HALF)
        own = pl.ds(pl.multiple_of(start + HALF, HALF), HALF)
        window = pl.ds(start, span)
        dq = jnp.broadcast_to(drow[0:1, own], (HALF, HALF)).T
        same = jnp.concatenate([dq, dq, dq], 1) == drow[0:1, window]
        ok = near & same
        keys = kv[window, :HEAD]
        vals = kv[window, HEAD:]
        for h in range(2):
            cols = slice(h * HEAD, (h + 1) * HEAD)
            s = lax.dot_general(
                q[pl.ds(start, HALF), cols],
                keys,
                (((1,), (1,)), ((), ())),
                preferred_element_type=F32,
            ) * HEAD ** (-0.5)
            s = jnp.where(ok, s, NEGATIVE)
            sink = sinks[0:1, h : h + 1]
            top = jnp.maximum(jnp.max(s, -1, keepdims=True), sink)
            w = jnp.exp(s - top)
            total = jnp.sum(w, -1, keepdims=True) + jnp.exp(sink - top)
            o = jnp.dot(w.astype(BF), vals, preferred_element_type=F32)
            out[:, cols] = (o / total).astype(BF)


def normalised(value):
    average = jnp.mean(value, -1, keepdims=True)
    centred = value - average
    variance = jnp.mean(centred * centred, -1, keepdims=True)
    return centred * lax.rsqrt(variance + EPS)


def chip(rz, ry):
    sp = lax.axis_index("sp")
    y, z = (sp // SP_Y) % 4, sp // SP_Z
    return pl.multiple_of(((z ^ rz) * 4 + (y ^ ry)) * 128, 128)


def norm_body(a0, a1, a3, a2, w_out, res, gain, out, nat, rot):
    x = lax.axis_index("tp")
    for n in range(0, D, 256):
        acc = ALPHA * res[:, n : n + 256].astype(F32)
        for mask, a in zip(ORDER, (a0, a1, a3, a2)):
            w = w_out[pl.ds(pl.multiple_of((x ^ mask) * 256, 256), 256), n : n + 256]
            acc = acc + jnp.dot(a[...], w, preferred_element_type=F32)
        nat[:, n : n + 256] = acc
    for s in range(0, OWN, 32):
        nat[s : s + 32, :] = normalised(nat[s : s + 32, :]) * gain[...]
    for t in range(0, D, 128):
        rot[:, t : t + 128] = pltpu.roll(nat[:, t : t + 128], 64, 1)
    low = lax.broadcasted_iota(jnp.int32, (OWN, 128), 1) < 64
    for i in range(4):
        for j in (0, 2):
            a, b = (pl.ds(chip(ORDER[i], ORDER[k]), 128) for k in (j, j + 1))
            dst = (i * 4 + j) * 64
            out[:, dst : dst + 128] = jnp.where(low, nat[:, a], rot[:, b]).astype(BF)
            a, b = (pl.ds(chip(ORDER[k], ORDER[i]), 128) for k in (j, j + 1))
            dst += 1024
            out[:, dst : dst + 128] = jnp.where(low, rot[:, a], nat[:, b]).astype(BF)


def product(rows, pieces, spans, acc, store):
    lhs = jnp.concatenate(
        [jnp.concatenate([r[:, a:b] for r in rows], 0) for a, b in spans], 1
    )
    for n in range(0, GU, 256):
        m = min(n + 256, GU)
        w = jnp.concatenate([p[:, n:m] for p in pieces], 0)
        t = jnp.dot(lhs, w, preferred_element_type=F32)
        store[:, n:m] = t if acc is None else acc[:, n:m] + t


def early_body(*refs):
    product(refs[:5], refs[5:17], ((0, 768), (1024, 1792)), None, refs[17])


def hidden_body(*refs):
    rows, pieces, early, out, acc = refs[:5], refs[5:9], refs[9], refs[10], refs[11]
    product(rows, pieces, ((768, 1024), (1792, 2048)), early, acc)
    live = lax.broadcasted_iota(jnp.int32, (64, DN), 1) < FFH
    for s in range(0, ROWS, 64):
        v = acc[s : s + 64, :]
        up = pltpu.roll(v, FFH, 1)[:, :DN]
        gate = v[:, :DN]
        h = gate / (1.0 + jnp.exp(-gate)) * up
        out[s : s + 64, :] = jnp.where(live, h, 0.0).astype(BF)


def down_parts(h, pieces):
    for i in range(0, len(pieces), 2):
        p = jnp.concatenate([r[:, r.shape[1] - DN :] for r in pieces[i : i + 2]], 0)
        at = i * 128
        yield (
            at,
            at + 256,
            lax.dot_general(h[...], p, (((1,), (1,)), ((), ())), preferred_element_type=F32),
        )


def give_body(h, *refs):
    pieces, out = refs[:-1], refs[-1]
    for a, b, v in down_parts(h, pieces):
        out[:, a:b] = v.astype(BF)


def take_body(h, theirs, *refs):
    pieces, (own, left, right, left_keep, right_keep) = refs[:-5], refs[-5:]
    half = own.shape[1] // 2
    for at, end, v in down_parts(h, pieces):
        v = v + theirs[:, at:end].astype(F32)
        b0, b1, b3, b2 = (v[k * OWN : (k + 1) * OWN, :] for k in range(4))
        own[:, at:end] = b0
        send, keep, near, away = (
            (left, left_keep, b1, b3) if at < half else (right, right_keep, b3, b1)
        )
        cols = slice(at % half, at % half + end - at)
        send[:OWN, cols] = near.astype(BF)
        send[OWN:, cols] = b2.astype(BF)
        keep[:, cols] = away


def fold_body(own, left, right, left_keep, right_keep, total, left_out, right_out):
    half = own.shape[1] // 2
    total[:, :half] = own[:, :half] + left[:OWN, :].astype(F32)
    total[:, half:] = own[:, half:] + right[:OWN, :].astype(F32)
    left_out[...] = (left_keep[...] + left[OWN:, :].astype(F32)).astype(BF)
    right_out[...] = (right_keep[...] + right[OWN:, :].astype(F32)).astype(BF)


def final_body(normed, gain, *refs):
    parts, out, pre = refs[:6], refs[6], refs[7]
    for c, (first, width) in enumerate(((0, 512), (512, 512))):
        total, *last = parts[3 * c : 3 * c + 3]
        for kind in range(2):
            dst = slice(kind * 1024 + first, kind * 1024 + first + width)
            n = normed[:, dst].astype(F32)
            v = total[:, kind * width : (kind + 1) * width] + last[kind][...].astype(F32)
            pre[:, dst] = ALPHA * n + v
    pre[...] = normalised(pre[...])
    low = lax.broadcasted_iota(jnp.int32, (OWN, 128), 1) < 64
    for i in range(4):
        for j in range(4):
            p, q = 4 * i + j, 4 * j + i
            a = pre[:, (p // 2) * 128 : (p // 2) * 128 + 128]
            b = pre[:, 1024 + (q // 2) * 128 : 1024 + (q // 2) * 128 + 128]
            if p % 2 == 1:
                a = pltpu.roll(a, 64, 1)
            if q % 2 == 0:
                b = pltpu.roll(b, 64, 1)
            at = pl.ds(chip(ORDER[i], ORDER[j]), 128)
            out[:, at] = (jnp.where(low, a, b) * gain[:, at]).astype(BF)


def spread(low_half, high_half, axis, low):
    one = swap(low_half, axis, low), swap(high_half, axis, low)
    three = swap(low_half, axis, 3 * low), swap(high_half, axis, 3 * low)

    def passed_on(cols):
        return (swap(one[0][:, cols], axis, 3 * low), swap(three[1][:, cols], axis, low))

    near = (low_half, high_half, *one, *three)
    return near, passed_on(slice(0, GU)), passed_on(slice(GU, GU + DN))


def per_device(
    queries,
    keys,
    values,
    doc_ids,
    sink_logit,
    residual_in,
    w_out,
    gain_one,
    w_gate,
    w_up,
    w_down,
    gain_two,
):
    core = lax.axis_index("sp") % 2
    local = (queries, keys, values, doc_ids.reshape(1, ROWS), sink_logit.reshape(1, 2))
    keep, send, inner, outer, *local = call(
        pack_body,
        (shape((64, GU + DN)),) * 2
        + (shape((HALF + 8, 2 * HEAD)),) * 2
        + tuple(shape(a.shape, a.dtype) for a in local),
        10**6,
        10**6,
        tuple(
            pltpu.with_memory_space_constraint(a, pltpu.HBM)
            for a in (w_gate, w_up, w_down.T, *local)
        ),
        [pltpu.VMEM((64, GU), BF)] * 3 + [pltpu.SemaphoreType.DMA((8,))],
        pltpu.HBM,
    )
    recv = swap(send, "sp", 1)
    from_0 = jnp.where(core == 0, keep, recv)
    from_1 = jnp.where(core == 0, recv, keep)

    side = swap(inner, "sp", 1)
    count = lax.axis_size("sp")
    pairs = [(i, i + 1) for i in range(1, count - 1, 2)]
    far = lax.ppermute(outer, "sp", pairs + [(b, a) for a, b in pairs])

    def columns(origin, near, across):
        units = ring(origin, "sp", near)
        halves = (jnp.concatenate(units[i : i + 2], 0) for i in (0, 2))
        return spread(*halves, "sp", across)

    near_a, gu_a, dn_a = columns(from_0, SP_Y, SP_Z)
    near_b, gu_b, dn_b = columns(from_1, SP_Z, SP_Y)

    attended = call(
        attend_body,
        (shape((OWN, 256)),) * 4,
        4 * ROWS * 256 * 384 * 8,
        10**6,
        (*local, side, far),
        (pltpu.VMEM((ROWS + 2 * HALF, 256), BF), pltpu.VMEM((8, ROWS + 2 * HALF), F32)),
    )
    atts = [swap(a, "tp", m) if m else a for m, a in zip(ORDER, attended)]
    normed = call(
        norm_body,
        shape((OWN, D)),
        2 * OWN * 1024 * D * 4,
        10**7,
        (*atts, w_out, residual_in, gain_one.reshape(1, D)),
        (pltpu.VMEM((OWN, D), F32),) * 2,
    )
    x1, x3 = swap(normed, "tp", 1), swap(normed, "tp", 3)
    mid = OWN // 2
    rows = (normed, x1, x3, swap(x1[:mid], "tp", 3), swap(x3[mid:], "tp", 1))
    others = [swap(r, "sp", 1) for r in rows]

    def hidden_of(r):
        early = call(
            early_body, shape((ROWS, GU), F32), 2 * ROWS * 1536 * GU, 10**7, (*r, *near_a, *near_b)
        )
        return call(
            hidden_body,
            shape((ROWS, DN)),
            2 * ROWS * 512 * GU,
            10**7,
            (*r, *gu_a, *gu_b, early),
            (pltpu.VMEM((ROWS, GU), F32),),
        )

    own_hidden, other_hidden = hidden_of(rows), hidden_of(others)
    sums = []
    chunks = [slice(0, 4), slice(4, 8)]
    all_a, all_b = (*near_a, *dn_a), (*near_b, *dn_b)
    for part_of in chunks:
        pieces = (*all_a[part_of], *all_b[part_of])
        width = 128 * len(pieces)
        flops = 2 * ROWS * DN * width
        part = call(give_body, shape((ROWS, width)), flops, 10**6, (other_hidden, *pieces))
        theirs = swap(part, "sp", 1)
        half = width // 2
        own, left, right, *keeps = call(
            take_body,
            (shape((OWN, width), F32),)
            + (shape((2 * OWN, half)),) * 2
            + (shape((OWN, half), F32),) * 2,
            flops,
            10**6,
            (own_hidden, theirs, *pieces),
        )
        left, right = swap(left, "tp", 1), swap(right, "tp", 3)
        own, left, right = call(
            fold_body,
            (shape((OWN, width), F32),) + (shape((OWN, half)),) * 2,
            10**6,
            10**6,
            (own, left, right, *keeps),
        )
        sums += [own, swap(left, "tp", 3), swap(right, "tp", 1)]
    return call(
        final_body,
        shape((OWN, D)),
        10**6,
        10**6,
        (normed, gain_two.reshape(1, D), *sums),
        (pltpu.VMEM((OWN, D), F32),),
    )


def solution(mesh):
    in_specs = (
        P("sp", "tp"),
        P("sp", "tp"),
        P("sp", "tp"),
        P("sp"),
        P("tp"),
        P(("sp", "tp"), None),
        P(),
        P(),
        P("sp", "tp"),
        P("sp", "tp"),
        P("tp", "sp"),
        P(),
    )
    out_specs = P(("sp", "tp"), None)
    return jax.shard_map(
        per_device, mesh=mesh, in_specs=in_specs, out_specs=out_specs, check_vma=False
    )
```

```python
import jax
import jax.numpy as jnp
from jax import lax
from jax.experimental import pallas as pl
from jax.experimental.pallas import tpu as pltpu
from jax.sharding import PartitionSpec as P


HEAD = 128
HALF = 128
ALPHA = 2.0**0.5
EPS = 1e-05
NEGATIVE = -1e30
BF, F32 = jnp.bfloat16, jnp.float32

ROWS = 512
OWN = 128
D = 2048
FFH = 704
GU = 2 * FFH
DN = 768
ORDER = (0, 1, 3, 2)
SP_Y, SP_Z = 2, 8


def swap(value, axis, mask):
    count = lax.axis_size(axis)
    return lax.ppermute(value, axis, [(i, i ^ mask) for i in range(count)])


def ring(value, axis, low):
    return [value] + [swap(value, axis, low * m) for m in ORDER[1:]]


def call(body, outs, flops, bytes_accessed, args, scratch=(), space=pltpu.VMEM, vmem_mib=20):
    vmem = pl.BlockSpec(memory_space=pltpu.VMEM)
    return pl.pallas_call(
        body,
        out_shape=outs,
        in_specs=[pl.BlockSpec(memory_space=space)] * len(args),
        out_specs=jax.tree.map(lambda _: vmem, outs),
        scratch_shapes=list(scratch),
        compiler_params=pltpu.CompilerParams(vmem_limit_bytes=vmem_mib << 20),
        cost_estimate=pl.CostEstimate(
            flops=flops, bytes_accessed=bytes_accessed, transcendentals=0
        ),
    )(*args)


def shape(dims, dtype=BF):
    return jax.ShapeDtypeStruct(dims, dtype)


def pack_body(
    gate, up, down, q, k, v, docs, sinks, *refs
):
    keep, send, side, far, q_o, k_o, v_o, docs_o, sinks_o, gate_v, up_v, down_v, sems = refs
    moves = [(gate, gate_v), (up, up_v), (down, down_v), (k, k_o), (v, v_o), (docs, docs_o)]
    moves += [(q, q_o), (sinks, sinks_o)]
    copies = [pltpu.make_async_copy(*m, sems.at[i]) for i, m in enumerate(moves)]
    for copy in copies:
        copy.start()
    zero = lax.axis_index("sp") % 2 == 0
    low = lax.broadcasted_iota(jnp.int32, (64, GU), 1) < FFH
    for copy in copies[:2]:
        copy.wait()
    g, u = gate_v[...].astype(F32), up_v[...].astype(F32)
    first = jnp.where(low, g, pltpu.roll(u, FFH, 1))
    second = jnp.where(low, pltpu.roll(g, FFH, 1), u)
    keep[:, :GU] = jnp.where(zero, first, second).astype(BF)
    send[:, :GU] = jnp.where(zero, second, first).astype(BF)
    copies[2].wait()
    d = down_v[...].astype(F32)
    d0 = jnp.where(low, d, 0.0)[:, :DN]
    d1 = jnp.where(low, pltpu.roll(d, FFH, 1), 0.0)[:, :DN]
    keep[:, GU:] = jnp.where(zero, d0, d1).astype(BF)
    send[:, GU:] = jnp.where(zero, d1, d0).astype(BF)
    for copy in copies[3:]:
        copy.wait()
    a, b = slice(0, HALF), slice(ROWS - HALF, ROWS)
    for out, end in ((side, zero), (far, jnp.logical_not(zero))):
        out[:HALF, :HEAD] = jnp.where(end, k_o[b, :], k_o[a, :])
        out[:HALF, HEAD:] = jnp.where(end, v_o[b, :], v_o[a, :])
        d = docs_o[...].astype(F32)
        d = jnp.where(end, d[:, b], d[:, a]).astype(BF)
        d = jnp.broadcast_to(d, (8, HALF))
        out[HALF:, :HEAD] = d
        out[HALF:, HEAD:] = d


def attend_body(q, k, v, docs, sinks, side, far, o0, o1, o3, o2, kv, drow):
    sp = lax.axis_index("sp")
    core = sp % 2
    zero = core == 0
    before = jnp.where(zero, far[...].astype(F32), side[...].astype(F32))
    after = jnp.where(zero, side[...].astype(F32), far[...].astype(F32))
    kv[0:HALF, :] = before[:HALF].astype(BF)
    kv[HALF : HALF + ROWS, :HEAD] = k[...]
    kv[HALF : HALF + ROWS, HEAD:] = v[...]
    kv[HALF + ROWS :, :] = after[:HALF].astype(BF)
    drow[:, 0:HALF] = jnp.where(sp == 0, -1.0, before[HALF:, :HALF])
    drow[:, HALF : HALF + ROWS] = jnp.broadcast_to(docs[...].astype(F32), (8, ROWS))
    drow[:, HALF + ROWS :] = jnp.where(
        sp == lax.axis_size("sp") - 1, -1.0, after[HALF:, :HALF]
    )
    span = 3 * HALF
    row = lax.broadcasted_iota(jnp.int32, (HALF, span), 0)
    col = lax.broadcasted_iota(jnp.int32, (HALF, span), 1)
    near = jnp.abs(col - HALF - row) <= HALF
    for mask, out in zip(ORDER, (o0, o1, o3, o2)):
        start = pl.multiple_of((lax.axis_index("tp") ^ mask) * HALF, HALF)
        own = pl.ds(pl.multiple_of(start + HALF, HALF), HALF)
        window = pl.ds(start, span)
        dq = jnp.broadcast_to(drow[0:1, own], (HALF, HALF)).T
        same = jnp.concatenate([dq, dq, dq], 1) == drow[0:1, window]
        ok = near & same
        keys = kv[window, :HEAD]
        vals = kv[window, HEAD:]
        for h in range(2):
            cols = slice(h * HEAD, (h + 1) * HEAD)
            s = lax.dot_general(
                q[pl.ds(start, HALF), cols],
                keys,
                (((1,), (1,)), ((), ())),
                preferred_element_type=F32,
            ) * HEAD ** (-0.5)
            s = jnp.where(ok, s, NEGATIVE)
            sink = sinks[0:1, h : h + 1]
            top = jnp.maximum(jnp.max(s, -1, keepdims=True), sink)
            w = jnp.exp(s - top)
            total = jnp.sum(w, -1, keepdims=True) + jnp.exp(sink - top)
            o = jnp.dot(w.astype(BF), vals, preferred_element_type=F32)
            out[:, cols] = (o / total).astype(BF)


def normalised(value):
    average = jnp.mean(value, -1, keepdims=True)
    centred = value - average
    variance = jnp.mean(centred * centred, -1, keepdims=True)
    return centred * lax.rsqrt(variance + EPS)


def chip(rz, ry):
    sp = lax.axis_index("sp")
    y, z = (sp // SP_Y) % 4, sp // SP_Z
    return pl.multiple_of(((z ^ rz) * 4 + (y ^ ry)) * 128, 128)


def norm_body(a0, a1, a3, a2, w_out, res, gain, out, nat, rot):
    x = lax.axis_index("tp")
    for n in range(0, D, 256):
        acc = ALPHA * res[:, n : n + 256].astype(F32)
        for mask, a in zip(ORDER, (a0, a1, a3, a2)):
            w = w_out[pl.ds(pl.multiple_of((x ^ mask) * 256, 256), 256), n : n + 256]
            acc = acc + jnp.dot(a[...], w, preferred_element_type=F32)
        nat[:, n : n + 256] = acc
    for s in range(0, OWN, 32):
        nat[s : s + 32, :] = normalised(nat[s : s + 32, :]) * gain[...]
    for t in range(0, D, 128):
        rot[:, t : t + 128] = pltpu.roll(nat[:, t : t + 128], 64, 1)
    low = lax.broadcasted_iota(jnp.int32, (OWN, 128), 1) < 64
    for i in range(4):
        for j in (0, 2):
            a, b = (pl.ds(chip(ORDER[i], ORDER[k]), 128) for k in (j, j + 1))
            dst = (i * 4 + j) * 64
            out[:, dst : dst + 128] = jnp.where(low, nat[:, a], rot[:, b]).astype(BF)
            a, b = (pl.ds(chip(ORDER[k], ORDER[i]), 128) for k in (j, j + 1))
            dst += 1024
            out[:, dst : dst + 128] = jnp.where(low, rot[:, a], nat[:, b]).astype(BF)


def product(rows, pieces, spans, acc, store):
    lhs = jnp.concatenate(
        [jnp.concatenate([r[:, a:b] for r in rows], 0) for a, b in spans], 1
    )
    for n in range(0, GU, 256):
        m = min(n + 256, GU)
        w = jnp.concatenate([p[:, n:m] for p in pieces], 0)
        t = jnp.dot(lhs, w, preferred_element_type=F32)
        store[:, n:m] = t if acc is None else acc[:, n:m] + t


def early_body(*refs):
    product(refs[:5], refs[5:17], ((0, 768), (1024, 1792)), None, refs[17])


def hidden_body(*refs):
    rows, pieces, early, out, acc = refs[:5], refs[5:9], refs[9], refs[10], refs[11]
    product(rows, pieces, ((768, 1024), (1792, 2048)), early, acc)
    live = lax.broadcasted_iota(jnp.int32, (64, DN), 1) < FFH
    for s in range(0, ROWS, 64):
        v = acc[s : s + 64, :]
        up = pltpu.roll(v, FFH, 1)[:, :DN]
        gate = v[:, :DN]
        h = gate / (1.0 + jnp.exp(-gate)) * up
        out[s : s + 64, :] = jnp.where(live, h, 0.0).astype(BF)


def down_parts(h, pieces):
    for i in range(0, len(pieces), 2):
        p = jnp.concatenate([r[:, r.shape[1] - DN :] for r in pieces[i : i + 2]], 0)
        at = i * 128
        yield (
            at,
            at + 256,
            lax.dot_general(h[...], p, (((1,), (1,)), ((), ())), preferred_element_type=F32),
        )


def give_body(h, *refs):
    pieces, out = refs[:-1], refs[-1]
    for a, b, v in down_parts(h, pieces):
        out[:, a:b] = v.astype(BF)


def hidden_give_body(*refs):
    inputs, pieces, (out, part, acc) = refs[:10], refs[10:-3], refs[-3:]
    hidden_body(*inputs, out, acc)
    give_body(out, *pieces, part)


def take_body(h, theirs, *refs):
    pieces, (own, left, right, left_keep, right_keep) = refs[:-5], refs[-5:]
    half = own.shape[1] // 2
    for at, end, v in down_parts(h, pieces):
        v = v + theirs[:, at:end].astype(F32)
        b0, b1, b3, b2 = (v[k * OWN : (k + 1) * OWN, :] for k in range(4))
        own[:, at:end] = b0
        send, keep, near, away = (
            (left, left_keep, b1, b3) if at < half else (right, right_keep, b3, b1)
        )
        cols = slice(at % half, at % half + end - at)
        send[:OWN, cols] = near.astype(BF)
        send[OWN:, cols] = b2.astype(BF)
        keep[:, cols] = away


def fold_body(own, left, right, left_keep, right_keep, total, left_out, right_out):
    half = own.shape[1] // 2
    total[:, :half] = own[:, :half] + left[:OWN, :].astype(F32)
    total[:, half:] = own[:, half:] + right[:OWN, :].astype(F32)
    left_out[...] = (left_keep[...] + left[OWN:, :].astype(F32)).astype(BF)
    right_out[...] = (right_keep[...] + right[OWN:, :].astype(F32)).astype(BF)


def final_body(normed, gain, *refs):
    parts, out, pre = refs[:6], refs[6], refs[7]
    for c, (first, width) in enumerate(((0, 512), (512, 512))):
        total, *last = parts[3 * c : 3 * c + 3]
        for kind in range(2):
            dst = slice(kind * 1024 + first, kind * 1024 + first + width)
            n = normed[:, dst].astype(F32)
            v = total[:, kind * width : (kind + 1) * width] + last[kind][...].astype(F32)
            pre[:, dst] = ALPHA * n + v
    pre[...] = normalised(pre[...])
    low = lax.broadcasted_iota(jnp.int32, (OWN, 128), 1) < 64
    for i in range(4):
        for j in range(4):
            p, q = 4 * i + j, 4 * j + i
            a = pre[:, (p // 2) * 128 : (p // 2) * 128 + 128]
            b = pre[:, 1024 + (q // 2) * 128 : 1024 + (q // 2) * 128 + 128]
            if p % 2 == 1:
                a = pltpu.roll(a, 64, 1)
            if q % 2 == 0:
                b = pltpu.roll(b, 64, 1)
            at = pl.ds(chip(ORDER[i], ORDER[j]), 128)
            out[:, at] = (jnp.where(low, a, b) * gain[:, at]).astype(BF)


def spread(low_half, high_half, axis, low):
    one = swap(low_half, axis, low), swap(high_half, axis, low)
    three = swap(low_half, axis, 3 * low), swap(high_half, axis, 3 * low)

    def passed_on(cols):
        return (swap(one[0][:, cols], axis, 3 * low), swap(three[1][:, cols], axis, low))

    near = (low_half, high_half, *one, *three)
    return near, passed_on(slice(0, GU)), passed_on(slice(GU, GU + DN))


def per_device(
    queries,
    keys,
    values,
    doc_ids,
    sink_logit,
    residual_in,
    w_out,
    gain_one,
    w_gate,
    w_up,
    w_down,
    gain_two,
):
    core = lax.axis_index("sp") % 2
    local = (queries, keys, values, doc_ids.reshape(1, ROWS), sink_logit.reshape(1, 2))
    keep, send, inner, outer, *local = call(
        pack_body,
        (shape((64, GU + DN)),) * 2
        + (shape((HALF + 8, 2 * HEAD)),) * 2
        + tuple(shape(a.shape, a.dtype) for a in local),
        10**6,
        10**6,
        tuple(
            pltpu.with_memory_space_constraint(a, pltpu.HBM)
            for a in (w_gate, w_up, w_down.T, *local)
        ),
        [pltpu.VMEM((64, GU), BF)] * 3 + [pltpu.SemaphoreType.DMA((8,))],
        pltpu.HBM,
    )
    recv = swap(send, "sp", 1)
    from_0 = jnp.where(core == 0, keep, recv)
    from_1 = jnp.where(core == 0, recv, keep)

    side = swap(inner, "sp", 1)
    count = lax.axis_size("sp")
    pairs = [(i, i + 1) for i in range(1, count - 1, 2)]
    far = lax.ppermute(outer, "sp", pairs + [(b, a) for a, b in pairs])

    def columns(origin, near, across):
        units = ring(origin, "sp", near)
        halves = (jnp.concatenate(units[i : i + 2], 0) for i in (0, 2))
        return spread(*halves, "sp", across)

    near_a, gu_a, dn_a = columns(from_0, SP_Y, SP_Z)
    near_b, gu_b, dn_b = columns(from_1, SP_Z, SP_Y)

    attended = call(
        attend_body,
        (shape((OWN, 256)),) * 4,
        4 * ROWS * 256 * 384 * 8,
        10**6,
        (*local, side, far),
        (pltpu.VMEM((ROWS + 2 * HALF, 256), BF), pltpu.VMEM((8, ROWS + 2 * HALF), F32)),
    )
    atts = [swap(a, "tp", m) if m else a for m, a in zip(ORDER, attended)]
    normed = call(
        norm_body,
        shape((OWN, D)),
        2 * OWN * 1024 * D * 4,
        10**7,
        (*atts, w_out, residual_in, gain_one.reshape(1, D)),
        (pltpu.VMEM((OWN, D), F32),) * 2,
    )
    x1, x3 = swap(normed, "tp", 1), swap(normed, "tp", 3)
    mid = OWN // 2
    rows = (normed, x1, x3, swap(x1[:mid], "tp", 3), swap(x3[mid:], "tp", 1))
    others = [swap(r, "sp", 1) for r in rows]

    def hidden_of(i, r):
        early = call(
            early_body, shape((ROWS, GU), F32), 2 * ROWS * 1536 * GU, 10**7, (*r, *near_a, *near_b)
        )
        first = (*near_a[:4], *near_b[:4]) if i else ()
        return call(
            hidden_give_body if i else hidden_body,
            (shape((ROWS, DN)), shape((ROWS, 1024))) if i else shape((ROWS, DN)),
            2 * ROWS * 512 * GU,
            10**7,
            (*r, *gu_a, *gu_b, early, *first),
            (pltpu.VMEM((ROWS, GU), F32),),
        )

    own_hidden = hidden_of(0, rows)
    other_hidden, part = hidden_of(1, others)
    sums = []
    chunks = [slice(0, 4), slice(4, 8)]
    all_a, all_b = (*near_a, *dn_a), (*near_b, *dn_b)
    for n, part_of in enumerate(chunks):
        pieces = (*all_a[part_of], *all_b[part_of])
        width = 128 * len(pieces)
        flops = 2 * ROWS * DN * width
        if n:
            args = (other_hidden, *pieces)
            part = call(give_body, shape((ROWS, width)), flops, 10**6, args)
        theirs = swap(part, "sp", 1)
        half = width // 2
        own, left, right, *keeps = call(
            take_body,
            (shape((OWN, width), F32),)
            + (shape((2 * OWN, half)),) * 2
            + (shape((OWN, half), F32),) * 2,
            flops,
            10**6,
            (own_hidden, theirs, *pieces),
        )
        left, right = swap(left, "tp", 1), swap(right, "tp", 3)
        own, left, right = call(
            fold_body,
            (shape((OWN, width), F32),) + (shape((OWN, half)),) * 2,
            10**6,
            10**6,
            (own, left, right, *keeps),
        )
        sums += [own, swap(left, "tp", 3), swap(right, "tp", 1)]
    return call(
        final_body,
        shape((OWN, D)),
        10**6,
        10**6,
        (normed, gain_two.reshape(1, D), *sums),
        (pltpu.VMEM((OWN, D), F32),),
    )


def solution(mesh):
    in_specs = (
        P("sp", "tp"),
        P("sp", "tp"),
        P("sp", "tp"),
        P("sp"),
        P("tp"),
        P(("sp", "tp"), None),
        P(),
        P(),
        P("sp", "tp"),
        P("sp", "tp"),
        P("tp", "sp"),
        P(),
    )
    out_specs = P(("sp", "tp"), None)
    return jax.shard_map(
        per_device, mesh=mesh, in_specs=in_specs, out_specs=out_specs, check_vma=False
    )
```
